32 devices in a mesh: kv: 8 (over z, y), tp: 4 (over x, core).
Axes of the slice: x: 2, y: 2, z: 4, core: 2. Of those that a mesh axis runs over, the one named last changes fastest.
Arguments:
- tokens: bfloat16 [4, 4096], P(None, 'kv'), may hold values from -70 to 70
- norm_gain: float32 [4096], P('kv'), may hold values from 0.1 to 1.9
- query_weight: bfloat16 [4096, 2048], P('kv', 'tp'), may hold values from -0.09375 to 0.09375
- key_weight: bfloat16 [4096, 256], P('kv', 'tp'), may hold values from -0.09375 to 0.09375
- value_weight: bfloat16 [4096, 256], P('kv', 'tp'), may hold values from -0.09375 to 0.09375
- cache_keys: bfloat16 [4, 2, 6144, 128], P(None, None, ('kv', 'tp')), may hold values from -480 to 480, as said below
- cache_values: bfloat16 [4, 2, 6144, 128], P(None, None, ('kv', 'tp')), may hold values from -6 to 6
- lengths: int32 [4], replicated, may hold values from 1536 to 6143
- lambdas: float32 [16], P('tp'), may hold values from 0.3 to 0.8
- head_gain: float32 [128], replicated, may hold values from 0.1 to 1.9
- output_weight: bfloat16 [2048, 4096], P('tp', 'kv'), may hold values from -0.125 to 0.125
Outputs:
- attended: bfloat16 [4, 4096], P(None, 'kv')
- new_keys: bfloat16 [4, 256], P(None, 'tp')
- new_values: bfloat16 [4, 256], P(None, 'tp')
The draws below stay inside these ranges and needn't reach their ends.
Inputs may be any that keep to these rules, and one draw needn't show every extreme that they name: `cache_keys`: of order 1.75 in most entries; some rows may be far larger.
All inputs are finite; a program needn't handle non-finite values.
Results may differ from the reference program's by a relative error of at most 0.038.
Values may be sent and summed in bfloat16 or wider, within the bound.
A program may use at most 64 MiB of HBM per device.

```python
import jax
import jax.numpy as jnp
from jax import lax

D = 4096
HEADS = 16
KV_HEADS = 2
QK = 64
VD = 128
SEQS = 4
POSITIONS = 6144
N_TP = 4


def draw_tokens(key, part):
    column = jnp.arange(D, dtype=jnp.float32)
    rising = jnp.exp(jnp.log(4.0) * column / D)
    values = jnp.clip(jax.random.normal(key, (SEQS, D), jnp.float32), -6.0, 6.0) * rising
    return values.astype(jnp.bfloat16)


def draw_cache_keys(key, part):
    drawn = 1.75 * jax.random.normal(key, (SEQS, KV_HEADS, POSITIONS, 2 * QK), jnp.float32)
    return jnp.clip(drawn, -480.0, 480.0).astype(jnp.bfloat16)


def set_ends(values, own_key, least, largest):
    index_at = [jax.random.randint(jax.random.fold_in(own_key, axis), (), 0, length) for axis, length in enumerate(values.shape)]
    widest = values.shape.index(max(values.shape))
    beside = index_at[:widest] + [(index_at[widest] + 1) % values.shape[widest]] + index_at[widest + 1:]
    return values.at[tuple(index_at)].set(least).at[tuple(beside)].set(largest)


def level_of(stream_key, dims, cuts, smallest, top_value):
    def one(dim, blocks):
        steps = jax.random.uniform(jax.random.fold_in(jax.random.fold_in(stream_key, 6), dim), (blocks,), jnp.float32, smallest / len(cuts), top_value / len(cuts))
        return jnp.repeat(jnp.exp(steps), dims[dim] // blocks).reshape((-1,) + (1,) * (len(dims) - dim - 1))

    loudness = one(*cuts[0])
    for cut in cuts[1:]:
        loudness = loudness * one(*cut)
    return loudness


def centred(key, extent, deviation, reach, cuts=(), kind=jnp.bfloat16):
    values = jax.random.normal(key, extent, jnp.float32) * deviation
    if len(cuts) > 0:
        values = level_of(key, extent, cuts, -0.22, 0.18) * values
    return jnp.clip(values, min=-reach, max=reach).astype(kind)


def setup_inputs(seed: int = 0) -> dict:
    seeds = jax.random.split(jax.random.key(seed), 12)
    return {
        "tokens": draw_tokens(jax.random.fold_in(seeds[11], 71), 0),
        "norm_gain": jnp.clip(1.0 + 0.18 * jax.random.normal(seeds[1], (D,), jnp.float32), 0.1, 1.9),
        "query_weight": centred(seeds[2], (D, HEADS * 2 * QK), D ** -0.5, 0.09375, ((0, 8), (1, 4))),
        "key_weight": centred(seeds[3], (D, KV_HEADS * 2 * QK), D ** -0.5, 0.09375, ((0, 8), (1, 4))),
        "value_weight": centred(seeds[4], (D, KV_HEADS * VD), D ** -0.5, 0.09375, ((0, 8), (1, 4))),
        "cache_keys": draw_cache_keys(jax.random.fold_in(seeds[11], 71), 0),
        "cache_values": centred(seeds[6], (SEQS, KV_HEADS, POSITIONS, VD), 1.0, 6.0, ((2, 32),)),
        "lengths": set_ends(jax.random.randint(seeds[7], (SEQS,), POSITIONS // 4, POSITIONS), jax.random.fold_in(seeds[7], 1), POSITIONS // 4, POSITIONS - 1).astype(jnp.int32),
        "lambdas": jnp.clip(0.3 + 0.5 * jax.random.uniform(seeds[8], (HEADS,), jnp.float32) ** level_of(seeds[8], (HEADS,), ((0, 4),), -0.2, 0.2), 0.3, 0.8),
        "head_gain": jnp.clip(1.0 + 0.18 * jax.random.normal(seeds[9], (VD,), jnp.float32), 0.1, 1.9),
        "output_weight": centred(seeds[10], (HEADS * VD, D), (HEADS * VD) ** -0.5, 0.125, ((0, 4), (1, 8))),
    }


NEG_FILL = -1e+30

def reference(tokens, norm_gain, query_weight, key_weight, value_weight, cache_keys, cache_values, lengths, lambdas, head_gain, output_weight):
    floats = tokens.astype(jnp.float32)
    squares = lax.optimization_barrier(jnp.sum(floats * floats, axis=1))
    inverse = lax.rsqrt(squares / D + 1e-06)[:, None]
    scaled = (floats * norm_gain).astype(jnp.bfloat16)
    queries = (jnp.dot(scaled, query_weight, preferred_element_type=jnp.float32) * inverse).astype(jnp.bfloat16)
    new_keys = (jnp.dot(scaled, key_weight, preferred_element_type=jnp.float32) * inverse).astype(jnp.bfloat16)
    new_values = (jnp.dot(scaled, value_weight, preferred_element_type=jnp.float32) * inverse).astype(jnp.bfloat16)
    group_size = HEADS // KV_HEADS
    query_rows = queries.astype(jnp.float32).reshape(SEQS, KV_HEADS, group_size, 2, QK)
    positions = jnp.arange(POSITIONS, dtype=jnp.int32)

    def one_sequence(inputs):
        query_row, key_rows, value_rows, length = inputs
        key_float = key_rows.astype(jnp.float32).reshape(KV_HEADS, POSITIONS, 2, QK)
        scores = jnp.einsum('hgcd,hpcd->hgcp', query_row, key_float) * QK ** (-0.5)
        live_mask = positions < length
        scores = jnp.where(live_mask, scores, NEG_FILL)
        peak = lax.optimization_barrier(jnp.max(scores, axis=-1, keepdims=True))
        weights = jnp.where(live_mask, jnp.exp(scores - peak), 0.0)
        totals = lax.optimization_barrier(jnp.sum(weights, axis=-1))
        rounded = lax.optimization_barrier(weights.astype(jnp.bfloat16)).astype(jnp.float32)
        summed = jnp.einsum('hgcp,hpv->hgcv', rounded, value_rows.astype(jnp.float32))
        return (summed / totals[..., None]).reshape(HEADS, 2, VD)
    ratios = lax.map(one_sequence, (query_rows, cache_keys, cache_values, lengths))
    mixed = ratios[:, :, 0] - lambdas[None, :, None] * ratios[:, :, 1]
    normed = mixed * lax.rsqrt(lax.optimization_barrier(jnp.mean(mixed * mixed, axis=-1, keepdims=True)) + 1e-06) * head_gain
    flattened = normed.astype(jnp.bfloat16).reshape(SEQS, HEADS * VD)
    rows_each = HEADS * VD // N_TP
    attended = jnp.zeros((SEQS, D), jnp.float32)
    for member in range(N_TP):
        partial_out = jnp.dot(flattened[:, member * rows_each:(member + 1) * rows_each], output_weight[member * rows_each:(member + 1) * rows_each], preferred_element_type=jnp.float32)
        attended = attended + lax.optimization_barrier(partial_out.astype(jnp.bfloat16)).astype(jnp.float32)
    return (attended.astype(jnp.bfloat16), new_keys, new_values)
```

```python
import functools

import jax
import jax.numpy as jnp
from jax import lax
from jax.experimental import pallas as pl
from jax.experimental.pallas import tpu as pltpu
from jax.sharding import PartitionSpec as P

MESH = pl.DeviceIdType.MESH
NEG_FILL = -1e30
LANES = 128
F32 = jnp.float32
BF16 = jnp.bfloat16


def kernel(
    dims,
    tokens,
    gain,
    query_weight,
    key_weight,
    value_weight,
    cache_keys,
    cache_values,
    lengths,
    lambdas,
    head_gain,
    output_weight,
    attended,
    new_keys,
    new_values,
    qw,
    kw,
    vw,
    ck,
    cv,
    ow,
    proj,
    qrows,
    qbuf,
    nsend,
    nbuf,
    abuf,
    nbuf2,
    abuf2,
    obuf,
    cols,
    load_sem,
    ps,
    pr,
    qs,
    qr,
    ns,
    nr,
    a_s,
    a_r,
    ns2,
    nr2,
    as2,
    ar2,
    os_,
    or_,
):
    n_kv, n_tp, width = dims
    seqs = tokens.shape[0]
    own_q = query_weight.shape[1]
    own_kv = key_weight.shape[1]
    heads = own_q // LANES
    kv_heads = cache_keys.shape[1]
    pos_count = cache_keys.shape[2]
    rows = 2 * heads * seqs
    tp_each = n_tp // kv_heads
    me_kv = lax.axis_index("kv")
    me_tp = lax.axis_index("tp")

    pairs = ((query_weight, qw), (key_weight, kw), (value_weight, vw),
             (cache_keys, ck), (cache_values, cv), (output_weight, ow))
    loads = [pltpu.make_async_copy(s, d, load_sem.at[i]) for i, (s, d) in enumerate(pairs)]
    for load in loads:
        load.start()

    kv_peers = [lax.rem(me_kv + d, n_kv) for d in range(1, n_kv)]
    tp_peers = [lax.rem(me_tp + d, n_tp) for d in range(1, n_tp)]

    barrier = pltpu.get_barrier_semaphore()
    for p in kv_peers:
        pl.semaphore_signal(barrier, inc=1, device_id=(p, me_tp), device_id_type=MESH)
    for p in tp_peers:
        pl.semaphore_signal(barrier, inc=1, device_id=(me_kv, p), device_id_type=MESH)

    def over_kv(buf, send, recv):
        return [
            pltpu.make_async_remote_copy(
                src_ref=buf.at[me_kv], dst_ref=buf.at[me_kv],
                send_sem=send.at[p], recv_sem=recv.at[me_kv],
                device_id=(p, me_tp), device_id_type=MESH,
            )
            for p in kv_peers
        ]

    def over_tp(buf, send, recv, source=None):
        return [
            pltpu.make_async_remote_copy(
                src_ref=buf.at[me_tp] if source is None else source.at[p],
                dst_ref=buf.at[me_tp],
                send_sem=send.at[p], recv_sem=recv.at[me_tp],
                device_id=(me_kv, p), device_id_type=MESH,
            )
            for p in tp_peers
        ]

    def arrived_kv(buf, send, recv):
        for p in kv_peers:
            pltpu.make_async_remote_copy(
                src_ref=buf.at[p], dst_ref=buf.at[p],
                send_sem=send.at[p], recv_sem=recv.at[p],
                device_id=(p, me_tp), device_id_type=MESH,
            ).wait_recv()

    def arrived_tp(buf, send, recv):
        for p in tp_peers:
            pltpu.make_async_remote_copy(
                src_ref=buf.at[p], dst_ref=buf.at[p],
                send_sem=send.at[p], recv_sem=recv.at[p],
                device_id=(me_kv, p), device_id_type=MESH,
            ).wait_recv()

    started = []

    def go(copies):
        for c in copies:
            c.start()
        started.extend(copies)

    floats = tokens[...].astype(F32)
    scaled = (floats * gain[...]).astype(BF16)
    squares = jnp.sum(floats * floats, axis=1, keepdims=True)
    high = squares.astype(BF16).astype(F32)
    lane4 = lax.broadcasted_iota(jnp.int32, (seqs, LANES), 1)
    proj[me_kv, :, proj.shape[2] - LANES:] = jnp.where(lane4 < 64, high, squares - high).astype(BF16)
    if own_q + 2 * own_kv < proj.shape[2] - LANES:
        gap = proj.shape[2] - LANES - own_q - 2 * own_kv
        proj[me_kv, :, own_q + 2 * own_kv:proj.shape[2] - LANES] = jnp.zeros((seqs, gap), BF16)
    for load in loads[:3]:
        load.wait()
    proj[me_kv, :, :own_q] = jnp.dot(scaled, qw[...], preferred_element_type=F32).astype(BF16)
    key_part = jnp.dot(scaled, kw[...], preferred_element_type=F32)
    value_part = jnp.dot(scaled, vw[...], preferred_element_type=F32)
    proj[me_kv, :, own_q:own_q + own_kv] = key_part.astype(BF16)
    proj[me_kv, :, own_q + own_kv:own_q + 2 * own_kv] = value_part.astype(BF16)
    pl.semaphore_wait(barrier, n_kv + n_tp - 2)
    go(over_kv(proj, ps, pr))

    half = rows * tp_each
    row_b = lax.rem(lax.broadcasted_iota(jnp.int32, (half, pos_count), 0), seqs)
    first = (me_kv * n_tp + me_tp) * pos_count
    position = first + lax.broadcasted_iota(jnp.int32, (half, pos_count), 1)
    limit = jnp.full((half, pos_count), lengths[0], jnp.int32)
    for b in range(1, seqs):
        limit = jnp.where(row_b == b, lengths[b], limit)
    live = position < limit
    lane_row = lax.broadcasted_iota(jnp.int32, (1, LANES), 1)
    within = lax.rem(lane_row, rows)
    factor = jnp.ones((1, LANES), F32)
    for j in range(heads):
        start = (heads + j) * seqs
        factor = jnp.where((within >= start) & (within < start + seqs), -lambdas[j], factor)

    arrived_kv(proj, ps, pr)
    total = proj[0].astype(F32)
    for k in range(1, n_kv):
        total = total + proj[k].astype(F32)
    base = total.shape[1] - LANES
    sq = total[:, base:base + 1] + total[:, base + 64:base + 65]
    inverse = lax.rsqrt(sq / width + 1e-06)
    for j in range(heads):
        qrows[j * seqs:(j + 1) * seqs, :] = total[:, j * LANES:(j + 1) * LANES] * inverse
    qbuf[me_tp] = qrows[...].astype(BF16)
    go(over_tp(qbuf, qs, qr))
    new_keys[...] = (total[:, own_q:own_q + own_kv] * inverse).astype(BF16)
    new_values[...] = (total[:, own_q + own_kv:own_q + 2 * own_kv] * inverse).astype(BF16)
    loads[3].wait()
    loads[4].wait()
    arrived_tp(qbuf, qs, qr)

    qlane = lax.broadcasted_iota(jnp.int32, (heads * seqs, LANES), 1)
    outs, peaks, sums = [], [], []
    for g in range(kv_heads):
        pieces = []
        for t in range(g * tp_each, (g + 1) * tp_each):
            q = qbuf[t].astype(F32) * 0.125
            pieces += [jnp.where(qlane < 64, q, 0.0), jnp.where(qlane >= 64, q, 0.0)]
        q_all = jnp.concatenate(pieces, axis=0).astype(BF16)
        scores = None
        for b in range(seqs):
            s = lax.dot_general(q_all, ck[b, g], (((1,), (1,)), ((), ())), preferred_element_type=F32)
            scores = s if b == 0 else jnp.where(row_b == b, s, scores)
        scores = jnp.where(live, scores, NEG_FILL)
        peak = jnp.max(scores, axis=1, keepdims=True)
        e = jnp.where(live, jnp.exp(scores - peak), 0.0)
        sums.append(jnp.sum(e, axis=1, keepdims=True))
        peaks.append(peak)
        acc = None
        for b in range(seqs):
            w = jnp.where(row_b == b, e, 0.0).astype(BF16)
            o = jnp.dot(w, cv[b, g], preferred_element_type=F32)
            acc = o if b == 0 else acc + o
        outs.append(acc)
    wide_lane = lax.broadcasted_iota(jnp.int32, (LANES, LANES), 1)
    peak_all = jnp.concatenate(peaks, axis=0)
    sum_all = jnp.concatenate(sums, axis=0)
    aux = jnp.where(wide_lane == 0, peak_all, jnp.where(wide_lane == 1, sum_all, 0.0)).T
    abuf[me_tp] = aux[0:2]
    go(over_tp(abuf, a_s, a_r))
    for g in range(kv_heads):
        for t in range(tp_each):
            nsend[g * tp_each + t] = outs[g][t * rows:(t + 1) * rows].astype(BF16)
    go(over_tp(nbuf, ns, nr, nsend))
    nbuf[me_tp] = nsend[me_tp]
    my_rows = pl.ds(pl.multiple_of(me_tp * rows, rows), rows)

    arrived_tp(abuf, a_s, a_r)
    m = [abuf[t, 0:1, :] for t in range(n_tp)]
    top = functools.reduce(jnp.maximum, m)
    scale = [jnp.exp(x - top) for x in m]
    denom = functools.reduce(jnp.add, [scale[t] * abuf[t, 1:2, :] for t in range(n_tp)])
    abuf2[me_kv, 0:1, :] = top
    abuf2[me_kv, 1:2, :] = denom
    go(over_kv(abuf2, as2, ar2))
    pad = [jnp.zeros((LANES - n_tp, LANES), F32)]
    cols[...] = jnp.concatenate(scale + pad, axis=0).T
    col = cols[my_rows, :]
    arrived_tp(nbuf, ns, nr)
    merged = functools.reduce(jnp.add, [col[:, t:t + 1] * nbuf[t].astype(F32) for t in range(n_tp)])
    nbuf2[me_kv] = merged.astype(BF16)
    go(over_kv(nbuf2, ns2, nr2))

    arrived_kv(abuf2, as2, ar2)
    m = [abuf2[k, 0:1, :] for k in range(n_kv)]
    top = functools.reduce(jnp.maximum, m)
    scale = [jnp.exp(x - top) for x in m]
    denom = functools.reduce(jnp.add, [scale[k] * abuf2[k, 1:2, :] for k in range(n_kv)])
    weight = factor / denom
    pad = [jnp.zeros((LANES - n_kv, LANES), F32)]
    cols[...] = jnp.concatenate([s * weight for s in scale] + pad, axis=0).T
    col = cols[my_rows, :]
    loads[5].wait()
    arrived_kv(nbuf2, ns2, nr2)
    ratio = functools.reduce(jnp.add, [col[:, k:k + 1] * nbuf2[k].astype(F32) for k in range(n_kv)])
    mixed = ratio[:rows // 2] + ratio[rows // 2:]
    normed = mixed * lax.rsqrt(jnp.mean(mixed * mixed, axis=1, keepdims=True) + 1e-06) * head_gain[...]
    qrows[...] = normed
    part = None
    for j in range(heads):
        x = qrows[j * seqs:(j + 1) * seqs, :].astype(BF16)
        o = jnp.dot(x, ow[j * LANES:(j + 1) * LANES, :], preferred_element_type=F32)
        part = o if j == 0 else part + o
    obuf[me_tp] = part.astype(BF16)
    go(over_tp(obuf, os_, or_))
    arrived_tp(obuf, os_, or_)
    out = obuf[0].astype(F32)
    for t in range(1, n_tp):
        out = out + obuf[t].astype(F32)
    attended[...] = out.astype(BF16)
    for c in started:
        c.wait_send()


def solution(mesh):
    n_kv, n_tp = mesh.shape["kv"], mesh.shape["tp"]

    def body(tokens, norm_gain, query_weight, key_weight, value_weight, cache_keys,
             cache_values, lengths, lambdas, head_gain, output_weight):
        seqs = tokens.shape[0]
        own_q = query_weight.shape[1]
        own_kv = key_weight.shape[1]
        heads = own_q // LANES
        rows = 2 * heads * seqs
        out_cols = output_weight.shape[1]
        side = -(-2 * own_kv // LANES) * LANES
        any_ = pl.BlockSpec(memory_space=pl.ANY)
        vmem = pl.BlockSpec(memory_space=pltpu.VMEM)
        smem = pl.BlockSpec(memory_space=pltpu.SMEM)
        dma = pltpu.SemaphoreType.DMA
        return pl.pallas_call(
            functools.partial(kernel, (n_kv, n_tp, tokens.shape[1] * n_kv)),
            out_shape=(
                jax.ShapeDtypeStruct((seqs, out_cols), BF16),
                jax.ShapeDtypeStruct((seqs, own_kv), BF16),
                jax.ShapeDtypeStruct((seqs, own_kv), BF16),
            ),
            in_specs=[vmem, vmem, any_, any_, any_, any_, any_, smem, smem, vmem, any_],
            out_specs=(vmem, vmem, vmem),
            scratch_shapes=[
                pltpu.VMEM(query_weight.shape, BF16),
                pltpu.VMEM(key_weight.shape, BF16),
                pltpu.VMEM(value_weight.shape, BF16),
                pltpu.VMEM(cache_keys.shape, BF16),
                pltpu.VMEM(cache_values.shape, BF16),
                pltpu.VMEM(output_weight.shape, BF16),
                pltpu.VMEM((n_kv, seqs, own_q + side + LANES), BF16),
                pltpu.VMEM((heads * seqs, LANES), F32),
                pltpu.VMEM((n_tp, heads * seqs, LANES), BF16),
                pltpu.VMEM((n_tp, rows, LANES), BF16),
                pltpu.VMEM((n_tp, rows, LANES), BF16),
                pltpu.VMEM((n_tp, 2, LANES), F32),
                pltpu.VMEM((n_kv, rows, LANES), BF16),
                pltpu.VMEM((n_kv, 2, LANES), F32),
                pltpu.VMEM((n_tp, seqs, out_cols), BF16),
                pltpu.VMEM((LANES, LANES), F32),
                dma((6,)),
                dma((n_kv,)), dma((n_kv,)),
                dma((n_tp,)), dma((n_tp,)),
                dma((n_tp,)), dma((n_tp,)),
                dma((n_tp,)), dma((n_tp,)),
                dma((n_kv,)), dma((n_kv,)),
                dma((n_kv,)), dma((n_kv,)),
                dma((n_tp,)), dma((n_tp,)),
            ],
            compiler_params=pltpu.CompilerParams(collective_id=0, has_side_effects=True),
        )(tokens, norm_gain[None, :], query_weight, key_weight, value_weight, cache_keys,
          cache_values, lengths, lambdas, head_gain[None, :], output_weight)

    return jax.shard_map(
        body,
        mesh=mesh,
        in_specs=(
            P(None, "kv"),
            P("kv"),
            P("kv", "tp"),
            P("kv", "tp"),
            P("kv", "tp"),
            P(None, None, ("kv", "tp"), None),
            P(None, None, ("kv", "tp"), None),
            P(),
            P("tp"),
            P(),
            P("tp", "kv"),
        ),
        out_specs=(P(None, "kv"), P(None, "tp"), P(None, "tp")),
        check_vma=False,
    )
```

```python
import functools

import jax
import jax.numpy as jnp
from jax import lax
from jax.experimental import pallas as pl
from jax.experimental.pallas import tpu as pltpu
from jax.sharding import PartitionSpec as P

MESH = pl.DeviceIdType.MESH
NEG_FILL = -1e30
LANES = 128
F32 = jnp.float32
BF16 = jnp.bfloat16


def kernel(
    dims,
    tokens_in,
    gain_in,
    query_weight,
    key_weight,
    value_weight,
    cache_keys,
    cache_values,
    lengths_in,
    lambdas_in,
    head_gain_in,
    output_weight,
    packed,
    tokens,
    gain,
    lengths,
    lambdas,
    head_gain,
    qw,
    kw,
    vw,
    ck,
    cv,
    ow,
    proj,
    qrows,
    qbuf,
    nsend,
    nbuf,
    abuf,
    nbuf2,
    abuf2,
    obuf,
    cols,
    load_sem,
    ps,
    pr,
    qs,
    qr,
    ns,
    nr,
    a_s,
    a_r,
    ns2,
    nr2,
    as2,
    ar2,
    os_,
    or_,
):
    n_kv, n_tp, width = dims
    seqs = tokens.shape[0]
    own_q = query_weight.shape[1]
    own_kv = key_weight.shape[0]
    out_cols = output_weight.shape[1]
    heads = own_q // LANES
    kv_heads = cache_keys.shape[1]
    pos_count = cache_keys.shape[2]
    rows = 2 * heads * seqs
    tp_each = n_tp // kv_heads
    me_kv = lax.axis_index("kv")
    me_tp = lax.axis_index("tp")

    kv_peers = [lax.rem(me_kv + d, n_kv) for d in range(1, n_kv)]
    tp_peers = [lax.rem(me_tp + d, n_tp) for d in range(1, n_tp)]

    barrier = pltpu.get_barrier_semaphore()
    for p in kv_peers:
        pl.semaphore_signal(barrier, inc=1, device_id=(p, me_tp), device_id_type=MESH)
    for p in tp_peers:
        pl.semaphore_signal(barrier, inc=1, device_id=(me_kv, p), device_id_type=MESH)

    pairs = ((tokens_in, tokens), (gain_in, gain), (query_weight, qw), (key_weight, kw),
             (value_weight, vw), (lengths_in, lengths), (lambdas_in, lambdas),
             (head_gain_in, head_gain), (cache_keys, ck), (cache_values, cv), (output_weight, ow))
    loads = [pltpu.make_async_copy(s, d, load_sem.at[i]) for i, (s, d) in enumerate(pairs)]
    for load in loads:
        load.start()

    def over_kv(buf, send, recv):
        return [
            pltpu.make_async_remote_copy(
                src_ref=buf.at[me_kv], dst_ref=buf.at[me_kv],
                send_sem=send.at[p], recv_sem=recv.at[me_kv],
                device_id=(p, me_tp), device_id_type=MESH,
            )
            for p in kv_peers
        ]

    def over_tp(buf, send, recv, source=None):
        return [
            pltpu.make_async_remote_copy(
                src_ref=buf.at[me_tp] if source is None else source.at[p],
                dst_ref=buf.at[me_tp],
                send_sem=send.at[p], recv_sem=recv.at[me_tp],
                device_id=(me_kv, p), device_id_type=MESH,
            )
            for p in tp_peers
        ]

    def arrived_kv(buf, send, recv):
        for p in kv_peers:
            pltpu.make_async_remote_copy(
                src_ref=buf.at[p], dst_ref=buf.at[p],
                send_sem=send.at[p], recv_sem=recv.at[p],
                device_id=(p, me_tp), device_id_type=MESH,
            ).wait_recv()

    def arrived_tp(buf, send, recv):
        for p in tp_peers:
            pltpu.make_async_remote_copy(
                src_ref=buf.at[p], dst_ref=buf.at[p],
                send_sem=send.at[p], recv_sem=recv.at[p],
                device_id=(me_kv, p), device_id_type=MESH,
            ).wait_recv()

    started = []

    def go(copies):
        for c in copies:
            c.start()
        started.extend(copies)

    for load in loads[:2]:
        load.wait()
    floats = tokens[...].astype(F32)
    scaled = (floats * gain[...]).astype(BF16)
    squares = jnp.sum(floats * floats, axis=1, keepdims=True)
    high = squares.astype(BF16).astype(F32)
    lane4 = lax.broadcasted_iota(jnp.int32, (seqs, LANES), 1)
    proj[me_kv, :, proj.shape[2] - LANES:] = jnp.where(lane4 < 64, high, squares - high).astype(BF16)
    if own_q + 2 * own_kv < proj.shape[2] - LANES:
        gap = proj.shape[2] - LANES - own_q - 2 * own_kv
        proj[me_kv, :, own_q + 2 * own_kv:proj.shape[2] - LANES] = jnp.zeros((seqs, gap), BF16)
    for load in loads[2:5]:
        load.wait()
    proj[me_kv, :, :own_q] = jnp.dot(scaled, qw[...], preferred_element_type=F32).astype(BF16)
    key_part = lax.dot_general(scaled, kw[...], (((1,), (1,)), ((), ())), preferred_element_type=F32)
    value_part = lax.dot_general(scaled, vw[...], (((1,), (1,)), ((), ())), preferred_element_type=F32)
    proj[me_kv, :, own_q:own_q + own_kv] = key_part.astype(BF16)
    proj[me_kv, :, own_q + own_kv:own_q + 2 * own_kv] = value_part.astype(BF16)
    pl.semaphore_wait(barrier, n_kv + n_tp - 2)
    go(over_kv(proj, ps, pr))

    for load in loads[5:8]:
        load.wait()
    half = rows * tp_each
    row_b = lax.rem(lax.broadcasted_iota(jnp.int32, (half, pos_count), 0), seqs)
    first = (me_kv * n_tp + me_tp) * pos_count
    position = first + lax.broadcasted_iota(jnp.int32, (half, pos_count), 1)
    limit = jnp.full((half, pos_count), lengths[0], jnp.int32)
    for b in range(1, seqs):
        limit = jnp.where(row_b == b, lengths[b], limit)
    live = position < limit
    lane_row = lax.broadcasted_iota(jnp.int32, (1, LANES), 1)
    within = lax.rem(lane_row, rows)
    factor = jnp.ones((1, LANES), F32)
    for j in range(heads):
        start = (heads + j) * seqs
        factor = jnp.where((within >= start) & (within < start + seqs), -lambdas[j], factor)

    arrived_kv(proj, ps, pr)
    total = proj[0].astype(F32)
    for k in range(1, n_kv):
        total = total + proj[k].astype(F32)
    base = total.shape[1] - LANES
    sq = total[:, base:base + 1] + total[:, base + 64:base + 65]
    inverse = lax.rsqrt(sq / width + 1e-06)
    for j in range(heads):
        qrows[j * seqs:(j + 1) * seqs, :] = total[:, j * LANES:(j + 1) * LANES] * inverse
    qbuf[me_tp] = qrows[...].astype(BF16)
    go(over_tp(qbuf, qs, qr))
    packed[:, out_cols:] = (total[:, own_q:own_q + 2 * own_kv] * inverse).astype(BF16)
    loads[8].wait()
    loads[9].wait()
    arrived_tp(qbuf, qs, qr)

    qlane = lax.broadcasted_iota(jnp.int32, (heads * seqs, LANES), 1)
    outs, peaks, sums = [], [], []
    for g in range(kv_heads):
        pieces = []
        for t in range(g * tp_each, (g + 1) * tp_each):
            q = qbuf[t].astype(F32) * 0.125
            pieces += [jnp.where(qlane < 64, q, 0.0), jnp.where(qlane >= 64, q, 0.0)]
        q_all = jnp.concatenate(pieces, axis=0).astype(BF16)
        scores = None
        for b in range(seqs):
            s = lax.dot_general(q_all, ck[b, g], (((1,), (1,)), ((), ())), preferred_element_type=F32)
            scores = s if b == 0 else jnp.where(row_b == b, s, scores)
        scores = jnp.where(live, scores, NEG_FILL)
        peak = jnp.max(scores, axis=1, keepdims=True)
        e = jnp.where(live, jnp.exp(scores - peak), 0.0)
        sums.append(jnp.sum(e, axis=1, keepdims=True))
        peaks.append(peak)
        acc = None
        for b in range(seqs):
            w = jnp.where(row_b == b, e, 0.0).astype(BF16)
            o = jnp.dot(w, cv[b, g], preferred_element_type=F32)
            acc = o if b == 0 else acc + o
        outs.append(acc)
    wide_lane = lax.broadcasted_iota(jnp.int32, (LANES, LANES), 1)
    peak_all = jnp.concatenate(peaks, axis=0)
    sum_all = jnp.concatenate(sums, axis=0)
    aux = jnp.where(wide_lane == 0, peak_all, jnp.where(wide_lane == 1, sum_all, 0.0)).T
    abuf[me_tp] = aux[0:2]
    go(over_tp(abuf, a_s, a_r))
    for g in range(kv_heads):
        for t in range(tp_each):
            nsend[g * tp_each + t] = outs[g][t * rows:(t + 1) * rows].astype(BF16)
    go(over_tp(nbuf, ns, nr, nsend))
    nbuf[me_tp] = nsend[me_tp]
    my_rows = pl.ds(pl.multiple_of(me_tp * rows, rows), rows)

    arrived_tp(abuf, a_s, a_r)
    m = [abuf[t, 0:1, :] for t in range(n_tp)]
    top = functools.reduce(jnp.maximum, m)
    scale = [jnp.exp(x - top) for x in m]
    denom = functools.reduce(jnp.add, [scale[t] * abuf[t, 1:2, :] for t in range(n_tp)])
    abuf2[me_kv, 0:1, :] = top
    abuf2[me_kv, 1:2, :] = denom
    go(over_kv(abuf2, as2, ar2))
    pad = [jnp.zeros((LANES - n_tp, LANES), F32)]
    cols[...] = jnp.concatenate(scale + pad, axis=0).T
    col = cols[my_rows, :]
    arrived_tp(nbuf, ns, nr)
    merged = functools.reduce(jnp.add, [col[:, t:t + 1] * nbuf[t].astype(F32) for t in range(n_tp)])
    nbuf2[me_kv] = merged.astype(BF16)
    go(over_kv(nbuf2, ns2, nr2))

    arrived_kv(abuf2, as2, ar2)
    m = [abuf2[k, 0:1, :] for k in range(n_kv)]
    top = functools.reduce(jnp.maximum, m)
    scale = [jnp.exp(x - top) for x in m]
    denom = functools.reduce(jnp.add, [scale[k] * abuf2[k, 1:2, :] for k in range(n_kv)])
    weight = factor / denom
    pad = [jnp.zeros((LANES - n_kv, LANES), F32)]
    cols[...] = jnp.concatenate([s * weight for s in scale] + pad, axis=0).T
    col = cols[my_rows, :]
    loads[10].wait()
    arrived_kv(nbuf2, ns2, nr2)
    ratio = functools.reduce(jnp.add, [col[:, k:k + 1] * nbuf2[k].astype(F32) for k in range(n_kv)])
    mixed = ratio[:rows // 2] + ratio[rows // 2:]
    normed = mixed * lax.rsqrt(jnp.mean(mixed * mixed, axis=1, keepdims=True) + 1e-06) * head_gain[...]
    qrows[...] = normed
    part = None
    for j in range(heads):
        x = qrows[j * seqs:(j + 1) * seqs, :].astype(BF16)
        o = jnp.dot(x, ow[j * LANES:(j + 1) * LANES, :], preferred_element_type=F32)
        part = o if j == 0 else part + o
    obuf[me_tp] = part.astype(BF16)
    go(over_tp(obuf, os_, or_))
    arrived_tp(obuf, os_, or_)
    out = obuf[0].astype(F32)
    for t in range(1, n_tp):
        out = out + obuf[t].astype(F32)
    packed[:, :out_cols] = out.astype(BF16)
    for c in started:
        c.wait_send()


def split(packed, attended, new_keys, new_values):
    cols, own = attended.shape[1], new_keys.shape[1]
    attended[...] = packed[:, :cols]
    rest = packed[:, cols:].astype(F32)
    new_keys[...] = rest[:, :own].astype(BF16)
    new_values[...] = rest[:, own:].astype(BF16)


def solution(mesh):
    n_kv, n_tp = mesh.shape["kv"], mesh.shape["tp"]

    def body(tokens, norm_gain, query_weight, key_weight, value_weight, cache_keys,
             cache_values, lengths, lambdas, head_gain, output_weight):
        seqs = tokens.shape[0]
        own_q = query_weight.shape[1]
        own_kv = key_weight.shape[1]
        heads = own_q // LANES
        rows = 2 * heads * seqs
        out_cols = output_weight.shape[1]
        side = -(-2 * own_kv // LANES) * LANES
        any_ = pl.BlockSpec(memory_space=pl.ANY)
        vmem = pl.BlockSpec(memory_space=pltpu.VMEM)
        dma = pltpu.SemaphoreType.DMA
        packed = pl.pallas_call(
            functools.partial(kernel, (n_kv, n_tp, tokens.shape[1] * n_kv)),
            out_shape=jax.ShapeDtypeStruct((seqs, out_cols + 2 * own_kv), BF16),
            in_specs=[any_] * 11,
            out_specs=vmem,
            scratch_shapes=[
                pltpu.VMEM(tokens.shape, BF16),
                pltpu.VMEM((1, tokens.shape[1]), F32),
                pltpu.SMEM(lengths.shape, jnp.int32),
                pltpu.SMEM(lambdas.shape, F32),
                pltpu.VMEM((1, LANES), F32),
                pltpu.VMEM(query_weight.shape, BF16),
                pltpu.VMEM(key_weight.shape[::-1], BF16),
                pltpu.VMEM(value_weight.shape[::-1], BF16),
                pltpu.VMEM(cache_keys.shape, BF16),
                pltpu.VMEM(cache_values.shape, BF16),
                pltpu.VMEM(output_weight.shape, BF16),
                pltpu.VMEM((n_kv, seqs, own_q + side + LANES), BF16),
                pltpu.VMEM((heads * seqs, LANES), F32),
                pltpu.VMEM((n_tp, heads * seqs, LANES), BF16),
                pltpu.VMEM((n_tp, rows, LANES), BF16),
                pltpu.VMEM((n_tp, rows, LANES), BF16),
                pltpu.VMEM((n_tp, 2, LANES), F32),
                pltpu.VMEM((n_kv, rows, LANES), BF16),
                pltpu.VMEM((n_kv, 2, LANES), F32),
                pltpu.VMEM((n_tp, seqs, out_cols), BF16),
                pltpu.VMEM((LANES, LANES), F32),
                dma((11,)),
                dma((n_kv,)), dma((n_kv,)),
                dma((n_tp,)), dma((n_tp,)),
                dma((n_tp,)), dma((n_tp,)),
                dma((n_tp,)), dma((n_tp,)),
                dma((n_kv,)), dma((n_kv,)),
                dma((n_kv,)), dma((n_kv,)),
                dma((n_tp,)), dma((n_tp,)),
            ],
            compiler_params=pltpu.CompilerParams(collective_id=0, has_side_effects=True),
        )(tokens, norm_gain[None, :], query_weight, key_weight.T, value_weight.T, cache_keys,
          cache_values, lengths, lambdas, head_gain[None, :], output_weight)
        return pl.pallas_call(
            split,
            out_shape=(
                jax.ShapeDtypeStruct((seqs, out_cols), BF16),
                jax.ShapeDtypeStruct((seqs, own_kv), BF16),
                jax.ShapeDtypeStruct((seqs, own_kv), BF16),
            ),
            in_specs=[vmem],
            out_specs=(vmem, vmem, vmem),
        )(packed)

    return jax.shard_map(
        body,
        mesh=mesh,
        in_specs=(
            P(None, "kv"),
            P("kv"),
            P("kv", "tp"),
            P("kv", "tp"),
            P("kv", "tp"),
            P(None, None, ("kv", "tp"), None),
            P(None, None, ("kv", "tp"), None),
            P(),
            P("tp"),
            P(),
            P("tp", "kv"),
        ),
        out_specs=(P(None, "kv"), P(None, "tp"), P(None, "tp")),
        check_vma=False,
    )
```

```python
import functools

import jax
import jax.numpy as jnp
from jax import lax
from jax.experimental import pallas as pl
from jax.experimental.pallas import tpu as pltpu
from jax.sharding import PartitionSpec as P

MESH = pl.DeviceIdType.MESH
NEG_FILL = -1e30
LANES = 128
F32 = jnp.float32
BF16 = jnp.bfloat16


def far_first(me, n):
    if n & (n - 1):
        return [lax.rem(me + d, n) for d in range(1, n)]
    bits = [1 << i for i in range(n.bit_length() - 1)]
    flips = {bit: bit * (1 - 2 * lax.rem(me // bit, 2)) for bit in bits}
    return [me + sum(flips[bit] for bit in bits if d & bit) for d in range(n - 1, 0, -1)]


def kernel(
    dims,
    tokens_in,
    gain_in,
    query_weight,
    key_weight,
    value_weight,
    cache_keys,
    cache_values,
    lengths_in,
    lambdas_in,
    head_gain_in,
    output_weight,
    packed,
    tokens,
    gain,
    lengths,
    lambdas,
    head_gain,
    qw,
    kw,
    vw,
    ck,
    cv,
    ow,
    proj,
    qrows,
    qbuf,
    nsend,
    nbuf,
    abuf,
    nbuf2,
    abuf2,
    obuf,
    cols,
    load_sem,
    ps,
    pr,
    qs,
    qr,
    ns,
    nr,
    a_s,
    a_r,
    ns2,
    nr2,
    as2,
    ar2,
    os_,
    or_,
):
    n_kv, n_tp, width = dims
    seqs = tokens.shape[0]
    own_q = query_weight.shape[1]
    own_kv = key_weight.shape[0]
    out_cols = output_weight.shape[1]
    heads = own_q // LANES
    kv_heads = cache_keys.shape[1]
    pos_count = cache_keys.shape[2]
    rows = 2 * heads * seqs
    tp_each = n_tp // kv_heads
    me_kv = lax.axis_index("kv")
    me_tp = lax.axis_index("tp")

    kv_peers = far_first(me_kv, n_kv)
    tp_peers = far_first(me_tp, n_tp)

    barrier = pltpu.get_barrier_semaphore()
    for p in kv_peers:
        pl.semaphore_signal(barrier, inc=1, device_id=(p, me_tp), device_id_type=MESH)
    for p in tp_peers:
        pl.semaphore_signal(barrier, inc=1, device_id=(me_kv, p), device_id_type=MESH)

    pairs = ((tokens_in, tokens), (gain_in, gain), (query_weight, qw), (key_weight, kw),
             (value_weight, vw), (lengths_in, lengths), (lambdas_in, lambdas),
             (head_gain_in, head_gain), (cache_keys, ck), (cache_values, cv), (output_weight, ow))
    loads = [pltpu.make_async_copy(s, d, load_sem.at[i]) for i, (s, d) in enumerate(pairs)]
    for load in loads:
        load.start()

    def over_kv(buf, send, recv):
        return [
            pltpu.make_async_remote_copy(
                src_ref=buf.at[me_kv], dst_ref=buf.at[me_kv],
                send_sem=send.at[p], recv_sem=recv.at[me_kv],
                device_id=(p, me_tp), device_id_type=MESH,
            )
            for p in kv_peers
        ]

    def over_tp(buf, send, recv, source=None):
        return [
            pltpu.make_async_remote_copy(
                src_ref=buf.at[me_tp] if source is None else source.at[p],
                dst_ref=buf.at[me_tp],
                send_sem=send.at[p], recv_sem=recv.at[me_tp],
                device_id=(me_kv, p), device_id_type=MESH,
            )
            for p in tp_peers
        ]

    def arrived_kv(buf, send, recv):
        for p in kv_peers:
            pltpu.make_async_remote_copy(
                src_ref=buf.at[p], dst_ref=buf.at[p],
                send_sem=send.at[p], recv_sem=recv.at[p],
                device_id=(p, me_tp), device_id_type=MESH,
            ).wait_recv()

    def arrived_tp(buf, send, recv):
        for p in tp_peers:
            pltpu.make_async_remote_copy(
                src_ref=buf.at[p], dst_ref=buf.at[p],
                send_sem=send.at[p], recv_sem=recv.at[p],
                device_id=(me_kv, p), device_id_type=MESH,
            ).wait_recv()

    started = []

    def go(copies):
        for c in copies:
            c.start()
        started.extend(copies)

    for load in loads[:2]:
        load.wait()
    floats = tokens[...].astype(F32)
    scaled = (floats * gain[...]).astype(BF16)
    squares = jnp.sum(floats * floats, axis=1, keepdims=True)
    high = squares.astype(BF16).astype(F32)
    lane4 = lax.broadcasted_iota(jnp.int32, (seqs, LANES), 1)
    proj[me_kv, :, proj.shape[2] - LANES:] = jnp.where(lane4 < 64, high, squares - high).astype(BF16)
    if own_q + 2 * own_kv < proj.shape[2] - LANES:
        gap = proj.shape[2] - LANES - own_q - 2 * own_kv
        proj[me_kv, :, own_q + 2 * own_kv:proj.shape[2] - LANES] = jnp.zeros((seqs, gap), BF16)
    for load in loads[2:5]:
        load.wait()
    proj[me_kv, :, :own_q] = jnp.dot(scaled, qw[...], preferred_element_type=F32).astype(BF16)
    key_part = lax.dot_general(scaled, kw[...], (((1,), (1,)), ((), ())), preferred_element_type=F32)
    value_part = lax.dot_general(scaled, vw[...], (((1,), (1,)), ((), ())), preferred_element_type=F32)
    proj[me_kv, :, own_q:own_q + own_kv] = key_part.astype(BF16)
    proj[me_kv, :, own_q + own_kv:own_q + 2 * own_kv] = value_part.astype(BF16)
    pl.semaphore_wait(barrier, n_kv + n_tp - 2)
    go(over_kv(proj, ps, pr))

    for load in loads[5:8]:
        load.wait()
    half = rows * tp_each
    row_b = lax.rem(lax.broadcasted_iota(jnp.int32, (half, pos_count), 0), seqs)
    first = (me_kv * n_tp + me_tp) * pos_count
    position = first + lax.broadcasted_iota(jnp.int32, (half, pos_count), 1)
    limit = jnp.full((half, pos_count), lengths[0], jnp.int32)
    for b in range(1, seqs):
        limit = jnp.where(row_b == b, lengths[b], limit)
    live = position < limit
    lane_row = lax.broadcasted_iota(jnp.int32, (1, LANES), 1)
    within = lax.rem(lane_row, rows)
    factor = jnp.ones((1, LANES), F32)
    for j in range(heads):
        start = (heads + j) * seqs
        factor = jnp.where((within >= start) & (within < start + seqs), -lambdas[j], factor)

    arrived_kv(proj, ps, pr)
    total = proj[0].astype(F32)
    for k in range(1, n_kv):
        total = total + proj[k].astype(F32)
    base = total.shape[1] - LANES
    sq = total[:, base:base + 1] + total[:, base + 64:base + 65]
    inverse = lax.rsqrt(sq / width + 1e-06)
    for j in range(heads):
        qrows[j * seqs:(j + 1) * seqs, :] = total[:, j * LANES:(j + 1) * LANES] * inverse
    qbuf[me_tp] = qrows[...].astype(BF16)
    go(over_tp(qbuf, qs, qr))
    packed[:, out_cols:] = (total[:, own_q:own_q + 2 * own_kv] * inverse).astype(BF16)
    loads[8].wait()
    loads[9].wait()
    arrived_tp(qbuf, qs, qr)

    qlane = lax.broadcasted_iota(jnp.int32, (heads * seqs, LANES), 1)
    outs, peaks, sums = [], [], []
    for g in range(kv_heads):
        pieces = []
        for t in range(g * tp_each, (g + 1) * tp_each):
            q = qbuf[t].astype(F32) * 0.125
            pieces += [jnp.where(qlane < 64, q, 0.0), jnp.where(qlane >= 64, q, 0.0)]
        q_all = jnp.concatenate(pieces, axis=0).astype(BF16)
        scores = None
        for b in range(seqs):
            s = lax.dot_general(q_all, ck[b, g], (((1,), (1,)), ((), ())), preferred_element_type=F32)
            scores = s if b == 0 else jnp.where(row_b == b, s, scores)
        scores = jnp.where(live, scores, NEG_FILL)
        peak = jnp.max(scores, axis=1, keepdims=True)
        e = jnp.where(live, jnp.exp(scores - peak), 0.0)
        sums.append(jnp.sum(e, axis=1, keepdims=True))
        peaks.append(peak)
        acc = None
        for b in range(seqs):
            w = jnp.where(row_b == b, e, 0.0).astype(BF16)
            o = jnp.dot(w, cv[b, g], preferred_element_type=F32)
            acc = o if b == 0 else acc + o
        outs.append(acc)
    wide_lane = lax.broadcasted_iota(jnp.int32, (LANES, LANES), 1)
    peak_all = jnp.concatenate(peaks, axis=0)
    sum_all = jnp.concatenate(sums, axis=0)
    aux = jnp.where(wide_lane == 0, peak_all, jnp.where(wide_lane == 1, sum_all, 0.0)).T
    abuf[me_tp] = aux[0:2]
    go(over_tp(abuf, a_s, a_r))
    for g in range(kv_heads):
        for t in range(tp_each):
            nsend[g * tp_each + t] = outs[g][t * rows:(t + 1) * rows].astype(BF16)
    go(over_tp(nbuf, ns, nr, nsend))
    nbuf[me_tp] = nsend[me_tp]
    my_rows = pl.ds(pl.multiple_of(me_tp * rows, rows), rows)

    arrived_tp(abuf, a_s, a_r)
    m = [abuf[t, 0:1, :] for t in range(n_tp)]
    top = functools.reduce(jnp.maximum, m)
    scale = [jnp.exp(x - top) for x in m]
    denom = functools.reduce(jnp.add, [scale[t] * abuf[t, 1:2, :] for t in range(n_tp)])
    abuf2[me_kv, 0:1, :] = top
    abuf2[me_kv, 1:2, :] = denom
    go(over_kv(abuf2, as2, ar2))
    pad = [jnp.zeros((LANES - n_tp, LANES), F32)]
    cols[...] = jnp.concatenate(scale + pad, axis=0).T
    col = cols[my_rows, :]
    arrived_tp(nbuf, ns, nr)
    merged = functools.reduce(jnp.add, [col[:, t:t + 1] * nbuf[t].astype(F32) for t in range(n_tp)])
    nbuf2[me_kv] = merged.astype(BF16)
    go(over_kv(nbuf2, ns2, nr2))

    arrived_kv(abuf2, as2, ar2)
    m = [abuf2[k, 0:1, :] for k in range(n_kv)]
    top = functools.reduce(jnp.maximum, m)
    scale = [jnp.exp(x - top) for x in m]
    denom = functools.reduce(jnp.add, [scale[k] * abuf2[k, 1:2, :] for k in range(n_kv)])
    weight = factor / denom
    pad = [jnp.zeros((LANES - n_kv, LANES), F32)]
    cols[...] = jnp.concatenate([s * weight for s in scale] + pad, axis=0).T
    col = cols[my_rows, :]
    loads[10].wait()
    arrived_kv(nbuf2, ns2, nr2)
    ratio = functools.reduce(jnp.add, [col[:, k:k + 1] * nbuf2[k].astype(F32) for k in range(n_kv)])
    mixed = ratio[:rows // 2] + ratio[rows // 2:]
    normed = mixed * lax.rsqrt(jnp.mean(mixed * mixed, axis=1, keepdims=True) + 1e-06) * head_gain[...]
    qrows[...] = normed
    part = None
    for j in range(heads):
        x = qrows[j * seqs:(j + 1) * seqs, :].astype(BF16)
        o = jnp.dot(x, ow[j * LANES:(j + 1) * LANES, :], preferred_element_type=F32)
        part = o if j == 0 else part + o
    obuf[me_tp] = part.astype(BF16)
    go(over_tp(obuf, os_, or_))
    arrived_tp(obuf, os_, or_)
    out = obuf[0].astype(F32)
    for t in range(1, n_tp):
        out = out + obuf[t].astype(F32)
    packed[:, :out_cols] = out.astype(BF16)
    for c in started:
        c.wait_send()


def split(packed, attended, new_keys, new_values):
    cols, own = attended.shape[1], new_keys.shape[1]
    attended[...] = packed[:, :cols]
    rest = packed[:, cols:].astype(F32)
    new_keys[...] = rest[:, :own].astype(BF16)
    new_values[...] = rest[:, own:].astype(BF16)


def solution(mesh):
    n_kv, n_tp = mesh.shape["kv"], mesh.shape["tp"]

    def body(tokens, norm_gain, query_weight, key_weight, value_weight, cache_keys,
             cache_values, lengths, lambdas, head_gain, output_weight):
        seqs = tokens.shape[0]
        own_q = query_weight.shape[1]
        own_kv = key_weight.shape[1]
        heads = own_q // LANES
        rows = 2 * heads * seqs
        out_cols = output_weight.shape[1]
        side = -(-2 * own_kv // LANES) * LANES
        any_ = pl.BlockSpec(memory_space=pl.ANY)
        vmem = pl.BlockSpec(memory_space=pltpu.VMEM)
        dma = pltpu.SemaphoreType.DMA
        packed = pl.pallas_call(
            functools.partial(kernel, (n_kv, n_tp, tokens.shape[1] * n_kv)),
            out_shape=pltpu.VMEM((seqs, out_cols + 2 * own_kv), BF16),
            in_specs=[any_] * 11,
            out_specs=vmem,
            scratch_shapes=[
                pltpu.VMEM(tokens.shape, BF16),
                pltpu.VMEM((1, tokens.shape[1]), F32),
                pltpu.SMEM(lengths.shape, jnp.int32),
                pltpu.SMEM(lambdas.shape, F32),
                pltpu.VMEM((1, LANES), F32),
                pltpu.VMEM(query_weight.shape, BF16),
                pltpu.VMEM(key_weight.shape[::-1], BF16),
                pltpu.VMEM(value_weight.shape[::-1], BF16),
                pltpu.VMEM(cache_keys.shape, BF16),
                pltpu.VMEM(cache_values.shape, BF16),
                pltpu.VMEM(output_weight.shape, BF16),
                pltpu.VMEM((n_kv, seqs, own_q + side + LANES), BF16),
                pltpu.VMEM((heads * seqs, LANES), F32),
                pltpu.VMEM((n_tp, heads * seqs, LANES), BF16),
                pltpu.VMEM((n_tp, rows, LANES), BF16),
                pltpu.VMEM((n_tp, rows, LANES), BF16),
                pltpu.VMEM((n_tp, 2, LANES), F32),
                pltpu.VMEM((n_kv, rows, LANES), BF16),
                pltpu.VMEM((n_kv, 2, LANES), F32),
                pltpu.VMEM((n_tp, seqs, out_cols), BF16),
                pltpu.VMEM((LANES, LANES), F32),
                dma((11,)),
                dma((n_kv,)), dma((n_kv,)),
                dma((n_tp,)), dma((n_tp,)),
                dma((n_tp,)), dma((n_tp,)),
                dma((n_tp,)), dma((n_tp,)),
                dma((n_kv,)), dma((n_kv,)),
                dma((n_kv,)), dma((n_kv,)),
                dma((n_tp,)), dma((n_tp,)),
            ],
            compiler_params=pltpu.CompilerParams(collective_id=0, has_side_effects=True),
        )(tokens, norm_gain[None, :], query_weight, key_weight.T, value_weight.T, cache_keys,
          cache_values, lengths, lambdas, head_gain[None, :], output_weight)
        return pl.pallas_call(
            split,
            out_shape=(
                jax.ShapeDtypeStruct((seqs, out_cols), BF16),
                jax.ShapeDtypeStruct((seqs, own_kv), BF16),
                jax.ShapeDtypeStruct((seqs, own_kv), BF16),
            ),
            in_specs=[vmem],
            out_specs=(vmem, vmem, vmem),
        )(pltpu.with_memory_space_constraint(packed, pltpu.VMEM))

    return jax.shard_map(
        body,
        mesh=mesh,
        in_specs=(
            P(None, "kv"),
            P("kv"),
            P("kv", "tp"),
            P("kv", "tp"),
            P("kv", "tp"),
            P(None, None, ("kv", "tp"), None),
            P(None, None, ("kv", "tp"), None),
            P(),
            P("tp"),
            P(),
            P("tp", "kv"),
        ),
        out_specs=(P(None, "kv"), P(None, "tp"), P(None, "tp")),
        check_vma=False,
    )
```
